32 devices in a mesh: rep: 4 (over z), fs: 2 (over y), tp: 4 (over x, core).
Axes of the slice: x: 2, y: 2, z: 4, core: 2. Of those that a mesh axis runs over, the one named last changes fastest.
Arguments:
- inputs: bfloat16 [2560, 2048], P('rep', 'fs'), may hold values from -6 to 6
- gate_pre: bfloat16 [2560, 5632], P('rep', 'tp'), may hold values from -12 to 12
- up_pre: bfloat16 [2560, 5632], P('rep', 'tp'), may hold values from -6 to 6
- cotangent: bfloat16 [2560, 2048], P('rep'), may hold values from -6 to 6
- w_gate: bfloat16 [2048, 5632], P('fs', 'tp'), may hold values from -0.125 to 0.125
- w_up: bfloat16 [2048, 5632], P('fs', 'tp'), may hold values from -0.125 to 0.125
- w_down: bfloat16 [5632, 2048], P('tp', 'fs'), may hold values from -0.078125 to 0.078125
Outputs:
- grad_input: bfloat16 [2560, 2048], P('rep', 'fs')
- grad_gate: float32 [512, 4, 5632], P('fs', 'rep', 'tp')
- grad_up: float32 [512, 4, 5632], P('fs', 'rep', 'tp')
- grad_down: float32 [5632, 512, 4], P('tp', 'fs', 'rep')
- gate_norms: float32 [512, 4], P('fs', 'rep')
- up_norms: float32 [512, 4], P('fs', 'rep')
- down_norms: float32 [5632], P('tp')
The draws below stay inside these ranges and needn't reach their ends.
All inputs are finite; a program needn't handle non-finite values.
Results may differ from the reference program's by a relative error of at most 0.02.
Values may be sent and summed in bfloat16 or wider, within the bound.
A program may use at most 64 MiB of HBM per device.

```python
import jax
import jax.numpy as jnp
from jax import lax

D = 2048
FF = 5632
TOKENS = 2560
N_REP = 4
N_TP = 4


def raised(values, key, source, target, shards_of, factor):
    def block_of(position):
        return (jnp.arange(values.shape[position]) // (values.shape[position] // shards_of)).reshape((-1,) + (1,) * (values.ndim - 1 - position))

    first = jax.random.permutation(key, shards_of)[block_of(target)]
    far = (block_of(target) + shards_of // 2) % shards_of
    return jnp.where((block_of(source) == first) | (block_of(source) == far), factor * values, values)


def level_of(own_key, shape, pieces, smallest, high):
    def one(dim, blocks):
        heights = jax.random.uniform(jax.random.fold_in(jax.random.fold_in(own_key, 6), dim), (blocks,), jnp.float32, smallest / len(pieces), high / len(pieces))
        return jnp.repeat(jnp.exp(heights), shape[dim] // blocks).reshape((-1,) + (1,) * (len(shape) - dim - 1))

    level = one(*pieces[0])
    for cut in pieces[1:]:
        level = level * one(*cut)
    return level


def bell_draw(own_key, shape, scale, bound, shards=(), kind=jnp.bfloat16):
    loudness = level_of(own_key, shape, shards, -0.22, 0.18) if shards else 1.0
    drawn = jax.random.normal(own_key, shape, jnp.float32) * scale * loudness
    return jnp.minimum(jnp.maximum(drawn, -bound), bound).astype(kind)


def heavy_noise(key, extent, deviation, most, pieces, heavy, held_as=jnp.bfloat16):
    entries = deviation * jax.random.normal(key, extent, jnp.float32)
    if pieces:
        entries = entries * level_of(key, extent, pieces, -0.22, 0.18)
    return jnp.clip(raised(entries, jax.random.fold_in(key, 3), *heavy), -most, most).astype(held_as)


def setup_inputs(seed: int = 0) -> dict:
    streams_of = jax.random.split(jax.random.key(seed), 8)
    return {
        "inputs": bell_draw(streams_of[0], (TOKENS, D), 1.0, 6.0, ((0, 4), (1, 2))),
        "gate_pre": bell_draw(streams_of[1], (TOKENS, FF), 2.0, 12.0, ((0, 4), (1, 4))),
        "up_pre": bell_draw(streams_of[2], (TOKENS, FF), 1.0, 6.0, ((0, 4), (1, 4))),
        "cotangent": heavy_noise(streams_of[3], (TOKENS, D), 1.0, 6.0, ((0, 4),), (0, 1, 4, 2.0)),
        "w_gate": bell_draw(streams_of[4], (D, FF), D ** -0.5, 0.125, ((0, 2), (1, 4))),
        "w_up": bell_draw(streams_of[5], (D, FF), D ** -0.5, 0.125, ((0, 2), (1, 4))),
        "w_down": bell_draw(streams_of[6], (FF, D), FF ** -0.5, 0.078125, ((0, 4), (1, 2))),
    }


def reference(inputs, gate_pre, up_pre, cotangent, w_gate, w_up, w_down):
    single = jnp.float32
    hidden_grad = jnp.dot(cotangent, w_down.T, preferred_element_type=single)
    gate = gate_pre.astype(single)
    upper = up_pre.astype(single)
    sigma = jax.nn.sigmoid(gate)
    active = gate * sigma
    hidden = (active * upper).astype(jnp.bfloat16)
    d_up = (hidden_grad * active).astype(jnp.bfloat16)
    d_gate = (hidden_grad * upper * sigma * (1.0 + gate * (1.0 - sigma))).astype(jnp.bfloat16)
    factor = float(TOKENS) ** -0.5
    grad_gate = jnp.dot(inputs.T, d_gate, preferred_element_type=single) * factor
    grad_up = jnp.dot(inputs.T, d_up, preferred_element_type=single) * factor
    grad_down = jnp.dot(hidden.T, cotangent, preferred_element_type=single) * factor
    block = FF // N_TP
    total = jnp.zeros(inputs.shape, single)
    for index in range(N_TP):
        lower = index * block
        term = jnp.dot(d_gate[:, lower:lower + block], w_gate[:, lower:lower + block].T, preferred_element_type=single)
        term = term + jnp.dot(d_up[:, lower:lower + block], w_up[:, lower:lower + block].T, preferred_element_type=single)
        term = lax.optimization_barrier(term.astype(jnp.bfloat16)).astype(single)
        total = total + term
    grad_input = total.astype(jnp.bfloat16)
    gate_norms = jnp.sum(grad_gate * grad_gate, axis=1).reshape(D // N_REP, N_REP)
    up_norms = jnp.sum(grad_up * grad_up, axis=1).reshape(D // N_REP, N_REP)
    down_norms = jnp.sum(grad_down * grad_down, axis=1)
    return (grad_input, grad_gate.reshape(D // N_REP, N_REP, FF), grad_up.reshape(D // N_REP, N_REP, FF),
            grad_down.reshape(FF, D // N_REP, N_REP), gate_norms, up_norms, down_norms)
```

```python
import functools

import jax
import jax.numpy as jnp
from jax import lax
from jax.experimental import pallas as pl
from jax.experimental.pallas import tpu as pltpu
from jax.sharding import PartitionSpec as P

LANES = 128
F32 = jnp.float32
BF16 = jnp.bfloat16
MESH = pl.DeviceIdType.MESH
NT = (((1,), (1,)), ((), ()))


def on_device(inputs, gate_pre, up_pre, cotangent, w_gate, w_up, w_down):
    single = jnp.float32
    groups = lax.axis_size("rep")
    width = w_down.shape[1]
    own_cot = lax.dynamic_slice_in_dim(cotangent, lax.axis_index("fs") * width, width, 1)
    partial_grad = jnp.einsum("td,fd->tf", own_cot, w_down, preferred_element_type=single)
    hidden_grad = lax.psum(partial_grad.astype(jnp.bfloat16), "fs").astype(jnp.float32)
    gate = gate_pre.astype(single)
    upper = up_pre.astype(single)
    sigma = jax.nn.sigmoid(gate)
    active = gate * sigma
    hidden = (active * upper).astype(jnp.bfloat16)
    d_up = (hidden_grad * active).astype(jnp.bfloat16)
    d_gate = (hidden_grad * upper * sigma * (1.0 + gate * (1.0 - sigma))).astype(jnp.bfloat16)
    factor = float(inputs.shape[0] * groups) ** (-0.5)
    owned = width // groups
    hunits = w_gate.shape[1]
    gate_local = jnp.einsum("td,tf->df", inputs, d_gate, preferred_element_type=single) * factor
    gate_parts = lax.all_to_all(
        gate_local.reshape(owned, groups, hunits).astype(jnp.bfloat16),
        "rep",
        split_axis=1,
        concat_axis=1,
        tiled=True,
    ).astype(jnp.float32)
    grad_gate = jnp.sum(gate_parts, axis=1, keepdims=True)
    up_local = jnp.einsum("td,tf->df", inputs, d_up, preferred_element_type=single) * factor
    up_parts = lax.all_to_all(
        up_local.reshape(owned, groups, hunits).astype(jnp.bfloat16),
        "rep",
        split_axis=1,
        concat_axis=1,
        tiled=True,
    ).astype(jnp.float32)
    grad_up = jnp.sum(up_parts, axis=1, keepdims=True)
    down_local = jnp.einsum("tf,td->fd", hidden, own_cot, preferred_element_type=single) * factor
    down_parts = lax.all_to_all(
        down_local.reshape(hunits, owned, groups).astype(jnp.bfloat16),
        "rep",
        split_axis=2,
        concat_axis=2,
        tiled=True,
    ).astype(jnp.float32)
    grad_down = jnp.sum(down_parts, axis=2, keepdims=True)
    input_term = jnp.einsum("tf,df->td", d_gate, w_gate, preferred_element_type=single)
    input_term = input_term + jnp.einsum("tf,df->td", d_up, w_up, preferred_element_type=single)
    grad_input = lax.psum(input_term.astype(jnp.bfloat16), "tp")
    gate_norms, up_norms = lax.psum(
        (jnp.sum(grad_gate * grad_gate, axis=2), jnp.sum(grad_up * grad_up, axis=2)), "tp"
    )
    down_norms = lax.psum(jnp.sum(grad_down * grad_down, axis=(1, 2)), ("rep", "fs"))
    return (grad_input, grad_gate, grad_up, grad_down, gate_norms, up_norms, down_norms)


def line_kernel(
    sizes, x_hbm, gate_hbm, up_hbm, cot_hbm, wg_hbm, wu_hbm, wd_hbm,
    gi_ref, out_ref, gu_norm_ref, down_norm_ref,
    x_ref, gate_ref, up_ref, cot_ref, wg_ref, wu_ref, wd_ref,
    left, right, pg_own, pg_peer, ab, bb, gi_acc, gi_own, gi_peer,
    gu_own, gu_peer, dn_own, dn_peer,
    load_sem, y_send, y_recv, a_send, a_recv, b_send, b_recv, c_send, c_recv,
    gi_send, gi_recv, gg_send, gg_recv, gn_send, gn_recv, dn_send, dn_recv,
):
    n_fs, n_tp, factor = sizes
    tokens, width = x_ref.shape
    hunits = gate_ref.shape[1]
    blocks = hunits // LANES
    items = 3 * blocks
    owned = width // 4
    share = tokens // n_tp
    rep, fs, tp = lax.axis_index("rep"), lax.axis_index("fs"), lax.axis_index("tp")
    side = rep // 2
    mid, end = 1 + side, 3 * side
    far_mid, far_end = 2 - side, 3 - 3 * side
    at_end = rep == end
    partner = mid + end - rep
    fs_peer = 1 - fs

    loads = [
        pltpu.make_async_copy(cot_hbm.at[:, pl.ds(pl.multiple_of(fs * width, LANES), width)], cot_ref, load_sem.at[0]),
        pltpu.make_async_copy(wd_hbm, wd_ref, load_sem.at[1]),
        pltpu.make_async_copy(gate_hbm, gate_ref, load_sem.at[2]),
        pltpu.make_async_copy(up_hbm, up_ref, load_sem.at[3]),
        pltpu.make_async_copy(x_hbm, x_ref, load_sem.at[4]),
        pltpu.make_async_copy(wg_hbm, wg_ref, load_sem.at[5]),
        pltpu.make_async_copy(wu_hbm, wu_ref, load_sem.at[6]),
    ]
    for load in loads:
        load.start()

    group = [(r, f) for r in range(4) for f in range(n_fs) if r or f]

    def in_group(step):
        return (lax.rem(rep + step[0], 4), lax.rem(fs + step[1], n_fs), tp)

    def in_tp(step):
        return (rep, fs, lax.rem(tp + step, n_tp))

    barrier = pltpu.get_barrier_semaphore()
    greeted = [in_group(s) for s in group] + [in_tp(s) for s in range(1, n_tp)]
    for other in greeted:
        pl.semaphore_signal(barrier, inc=1, device_id=other, device_id_type=MESH)
    pl.semaphore_wait(barrier, len(greeted))

    def remote(src, dst, send, recv, other):
        return pltpu.make_async_remote_copy(
            src_ref=src, dst_ref=dst, send_sem=send, recv_sem=recv, device_id=other, device_id_type=MESH
        )

    def y_copy(j):
        return remote(pg_own.at[j], pg_peer.at[j], y_send.at[j], y_recv.at[j], (rep, fs_peer, tp))

    def a_copy(t):
        return remote(ab.at[t], ab.at[t], a_send.at[t], a_recv.at[t], (partner, fs, tp))

    def b_copy(t):
        return remote(ab.at[t, pl.ds(owned, 2 * owned)], bb.at[t], b_send.at[t], b_recv.at[t], (far_mid, fs, tp))

    def c_copy(t):
        return remote(
            bb.at[t, pl.ds(owned, owned)], bb.at[t, pl.ds(0, owned)], c_send.at[t], c_recv.at[t], (partner, fs, tp)
        )

    def lanes(j):
        return pl.ds(pl.multiple_of(j * LANES, LANES), LANES)

    def term(kind, owner, t):
        rows = pl.ds(pl.multiple_of(owner * owned, owned), owned)
        return jnp.dot(left[kind, rows, :], right[t], preferred_element_type=F32) * factor

    def loop(first, last, body):
        def step(i, carry):
            body(i)
            return carry
        lax.fori_loop(first, last, step, 0)

    loads[0].wait()
    loads[1].wait()

    def partial_of(j):
        rows = pl.ds(pl.multiple_of(j * LANES, LANES), LANES)
        pg_own[j] = lax.dot_general(cot_ref[...], wd_ref[rows, :], NT, preferred_element_type=F32).astype(BF16)
        y_copy(j).start()

    loop(0, blocks, partial_of)

    def spread(kind, source):
        for b in range(4):
            place = lax.broadcasted_iota(jnp.int32, (owned, width), 0) * 4 + b
            pick = (place == lax.broadcasted_iota(jnp.int32, (owned, width), 1)).astype(F32).astype(BF16)
            left[kind, b * owned:(b + 1) * owned, :] = lax.dot_general(
                pick, source[...], NT, preferred_element_type=F32
            ).astype(BF16)

    spread(0, cot_ref)
    loads[2].wait()
    loads[3].wait()

    def send_first(kind, t):
        for slot, owner in enumerate((mid, far_mid, far_end)):
            ab[t, slot * owned:(slot + 1) * owned, :] = term(kind, owner, t).astype(BF16)
        a_copy(t).start()

    def hidden_of(j):
        g = gate_ref[:, lanes(j)].astype(F32)
        u = up_ref[:, lanes(j)].astype(F32)
        right[j] = (g * (1.0 / (1.0 + jnp.exp(-g))) * u).astype(BF16)

        @pl.when(at_end)
        def _():
            send_first(0, j)

    loop(0, blocks, hidden_of)
    loads[4].wait()
    spread(1, x_ref)

    def pass_on(kind, t):
        a_copy(t).wait_recv()
        for slot, owner in ((1, far_mid), (2, far_end)):
            rows = slice(slot * owned, (slot + 1) * owned)
            ab[t, rows, :] = (ab[t, rows, :].astype(F32) + term(kind, owner, t)).astype(BF16)
        b_copy(t).start()

    def settle(kind, t):
        b_copy(t).wait_recv()
        bb[t, owned:, :] = (bb[t, owned:, :].astype(F32) + term(kind, end, t)).astype(BF16)
        c_copy(t).start()
        both = ab[t, :owned, :].astype(F32) + bb[t, :owned, :].astype(F32)
        out_ref[t] = both + term(kind, mid, t)

    def last_hop(kind, t):
        c_copy(t).wait_recv()
        out_ref[t] = bb[t, :owned, :].astype(F32) + term(kind, end, t)

    lag = 2

    def line(kind, first, last):
        for t in range(first, first + lag):
            pass_on(kind, t)

        def step(t):
            pass_on(kind, t)
            settle(kind, t - lag)

        loop(first + lag, last, step)

    @pl.when(jnp.logical_not(at_end))
    def _():
        line(0, 0, blocks)

    def grads_of(j):
        y_copy(j).wait_recv()
        g = gate_ref[:, lanes(j)].astype(F32)
        u = up_ref[:, lanes(j)].astype(F32)
        total = pg_own[j].astype(F32) + pg_peer[j].astype(F32)
        s = 1.0 / (1.0 + jnp.exp(-g))
        t = blocks + 2 * j
        right[t] = (total * u * s * (1.0 + g * (1.0 - s))).astype(BF16)
        right[t + 1] = (total * (g * s)).astype(BF16)

        @pl.when(at_end)
        def _():
            send_first(1, t)
            send_first(1, t + 1)

    loop(0, blocks, grads_of)

    loads[5].wait()
    loads[6].wait()
    gi_acc[...] = jnp.zeros_like(gi_acc)

    def gi_term(j):
        t = blocks + 2 * j
        gi_acc[...] += lax.dot_general(right[t], wg_ref[:, lanes(j)], NT, preferred_element_type=F32) + lax.dot_general(
            right[t + 1], wu_ref[:, lanes(j)], NT, preferred_element_type=F32
        )

    loop(0, blocks, gi_term)
    gi_own[...] = gi_acc[...].astype(BF16)

    def tokens_of(owner):
        return pl.ds(pl.multiple_of(owner * share, share), share)

    def gi_copy(step):
        other = lax.rem(tp + step, n_tp)
        return remote(
            gi_own.at[tokens_of(other)], gi_peer.at[step - 1], gi_send.at[step - 1], gi_recv.at[step - 1], in_tp(step)
        )

    def gg_copy(step):
        return remote(
            gi_ref.at[tokens_of(tp)], gi_ref.at[tokens_of(tp)], gg_send.at[step - 1], gg_recv.at[step - 1], in_tp(step)
        )

    for step in range(1, n_tp):
        gi_copy(step).start()

    half = blocks + 2 * (blocks // 2)

    @pl.when(at_end)
    def _():
        loop(0, blocks, functools.partial(last_hop, 0))

    @pl.when(jnp.logical_not(at_end))
    def _():
        for t in range(blocks - lag, blocks):
            settle(0, t)
        line(1, blocks, half)

    dn_own[...] = jnp.zeros_like(dn_own)
    for j in range(blocks):
        piece = out_ref[j]
        dn_own[0:1, j * LANES:(j + 1) * LANES] = jnp.sum(piece * piece, axis=0, keepdims=True)

    def dn_copy(k):
        return remote(dn_own, dn_peer.at[k], dn_send.at[k], dn_recv.at[k], in_group(group[k]))

    for k in range(len(group)):
        dn_copy(k).start()

    for step in range(1, n_tp):
        gi_copy(step).wait_recv()
    whole = gi_own[tokens_of(tp), :].astype(F32)
    for step in range(1, n_tp):
        whole += gi_peer[step - 1].astype(F32)
    gi_ref[tokens_of(tp), :] = whole.astype(BF16)
    for step in range(1, n_tp):
        gg_copy(step).start()

    @pl.when(at_end)
    def _():
        loop(blocks, items, functools.partial(last_hop, 1))

    @pl.when(jnp.logical_not(at_end))
    def _():
        def step(t):
            pass_on(1, t)
            settle(1, t - lag)

        loop(half, items, step)
        for t in range(items - lag, items):
            settle(1, t)

    gu_own[...] = jnp.zeros_like(gu_own)
    for kind in range(2):
        squares = jnp.zeros((owned, LANES), F32)
        for j in range(blocks):
            piece = out_ref[blocks + 2 * j + kind]
            squares += piece * piece
        gu_own[kind:kind + 1, :] = jnp.sum(squares.T, axis=0, keepdims=True)

    def gn_copy(step):
        return remote(gu_own, gu_peer.at[step - 1], gn_send.at[step - 1], gn_recv.at[step - 1], in_tp(step))

    for step in range(1, n_tp):
        gn_copy(step).start()

    for k in range(len(group)):
        dn_copy(k).wait_recv()
    down = dn_own[...]
    for k in range(len(group)):
        down += dn_peer[k]
    down_norm_ref[...] = down

    for step in range(1, n_tp):
        gn_copy(step).wait_recv()
    gate_up = gu_own[...]
    for step in range(1, n_tp):
        gate_up += gu_peer[step - 1]
    gu_norm_ref[...] = gate_up

    for step in range(1, n_tp):
        gg_copy(step).wait_recv()
        gg_copy(step).wait_send()
        gi_copy(step).wait_send()
        gn_copy(step).wait_send()
    for k in range(len(group)):
        dn_copy(k).wait_send()
    loop(0, blocks, lambda j: y_copy(j).wait_send())

    @pl.when(at_end)
    def _():
        loop(0, items, lambda t: a_copy(t).wait_send())

    @pl.when(jnp.logical_not(at_end))
    def _():
        def drain(t):
            b_copy(t).wait_send()
            c_copy(t).wait_send()

        loop(0, items, drain)


def on_line(inputs, gate_pre, up_pre, cotangent, w_gate, w_up, w_down):
    n_fs, n_tp = lax.axis_size("fs"), lax.axis_size("tp")
    tokens, width = inputs.shape
    hunits = w_gate.shape[1]
    blocks = hunits // LANES
    items = 3 * blocks
    owned = width // 4
    share = tokens // n_tp
    n_group = 4 * n_fs - 1
    dma = pltpu.SemaphoreType.DMA
    vmem = pltpu.VMEM
    sizes = (n_fs, n_tp, float(tokens * 4) ** (-0.5))
    grad_input, parts, gate_up, down = pl.pallas_call(
        functools.partial(line_kernel, sizes),
        out_shape=(
            jax.ShapeDtypeStruct((tokens, width), BF16),
            jax.ShapeDtypeStruct((items, owned, LANES), F32),
            jax.ShapeDtypeStruct((8, owned), F32),
            jax.ShapeDtypeStruct((8, hunits), F32),
        ),
        in_specs=[pl.BlockSpec(memory_space=pl.ANY)] * 7,
        out_specs=(pl.BlockSpec(memory_space=vmem),) * 4,
        scratch_shapes=[
            vmem((tokens, width), BF16),
            vmem((tokens, hunits), BF16),
            vmem((tokens, hunits), BF16),
            vmem((tokens, width), BF16),
            vmem((width, hunits), BF16),
            vmem((width, hunits), BF16),
            vmem((hunits, width), BF16),
            vmem((2, width, tokens), BF16),
            vmem((items, tokens, LANES), BF16),
            vmem((blocks, tokens, LANES), BF16),
            vmem((blocks, tokens, LANES), BF16),
            vmem((items, 3 * owned, LANES), BF16),
            vmem((items, 2 * owned, LANES), BF16),
            vmem((tokens, width), F32),
            vmem((tokens, width), BF16),
            vmem((n_tp - 1, share, width), BF16),
            vmem((8, owned), F32),
            vmem((n_tp - 1, 8, owned), F32),
            vmem((8, hunits), F32),
            vmem((n_group, 8, hunits), F32),
            dma((7,)),
            dma((blocks,)), dma((blocks,)),
            dma((items,)), dma((items,)),
            dma((items,)), dma((items,)),
            dma((items,)), dma((items,)),
            dma((n_tp - 1,)), dma((n_tp - 1,)),
            dma((n_tp - 1,)), dma((n_tp - 1,)),
            dma((n_tp - 1,)), dma((n_tp - 1,)),
            dma((n_group,)), dma((n_group,)),
        ],
        compiler_params=pltpu.CompilerParams(
            collective_id=0, has_side_effects=True, vmem_limit_bytes=67043328
        ),
    )(inputs, gate_pre, up_pre, cotangent, w_gate, w_up, w_down)
    grad_down = parts[:blocks].transpose(0, 2, 1).reshape(hunits, owned, 1)
    pairs = parts[blocks:].reshape(blocks, 2, owned, LANES)
    grad_gate = pairs[:, 0].transpose(1, 0, 2).reshape(owned, 1, hunits)
    grad_up = pairs[:, 1].transpose(1, 0, 2).reshape(owned, 1, hunits)
    return (
        grad_input,
        grad_gate,
        grad_up,
        grad_down,
        gate_up[0].reshape(owned, 1),
        gate_up[1].reshape(owned, 1),
        down[0],
    )


def fits_line(mesh, inputs, w_gate):
    n_rep, n_fs, n_tp = (mesh.shape[axis] for axis in ("rep", "fs", "tp"))
    tokens, width = inputs.shape[0] // n_rep, inputs.shape[1] // n_fs
    return (
        n_rep == 4 and n_fs == 2 and n_tp > 1
        and tokens % (16 * n_tp) == 0 and tokens % LANES == 0
        and width % (4 * LANES) == 0 and (w_gate.shape[1] // n_tp) % LANES == 0
    )


def solution(mesh):
    placed = (
        P("rep", "fs"),
        P("rep", "tp"),
        P("rep", "tp"),
        P("rep", None),
        P("fs", "tp"),
        P("fs", "tp"),
        P("tp", "fs"),
    )
    out_placed = (
        P("rep", "fs"),
        P("fs", "rep", "tp"),
        P("fs", "rep", "tp"),
        P("tp", "fs", "rep"),
        P("fs", "rep"),
        P("fs", "rep"),
        P("tp"),
    )

    def whole(inputs, gate_pre, up_pre, cotangent, w_gate, w_up, w_down):
        body = on_line if fits_line(mesh, inputs, w_gate) else on_device
        mapped = jax.shard_map(body, mesh=mesh, in_specs=placed, out_specs=out_placed, check_vma=False)
        return mapped(inputs, gate_pre, up_pre, cotangent, w_gate, w_up, w_down)

    return whole
```

```python
import functools

import jax
import jax.numpy as jnp
from jax import lax
from jax.experimental import pallas as pl
from jax.experimental.pallas import tpu as pltpu
from jax.sharding import PartitionSpec as P

LANES = 128
F32 = jnp.float32
BF16 = jnp.bfloat16
MESH = pl.DeviceIdType.MESH
NT = (((1,), (1,)), ((), ()))


def on_device(inputs, gate_pre, up_pre, cotangent, w_gate, w_up, w_down):
    single = jnp.float32
    groups = lax.axis_size("rep")
    width = w_down.shape[1]
    own_cot = lax.dynamic_slice_in_dim(cotangent, lax.axis_index("fs") * width, width, 1)
    partial_grad = jnp.einsum("td,fd->tf", own_cot, w_down, preferred_element_type=single)
    hidden_grad = lax.psum(partial_grad.astype(jnp.bfloat16), "fs").astype(jnp.float32)
    gate = gate_pre.astype(single)
    upper = up_pre.astype(single)
    sigma = jax.nn.sigmoid(gate)
    active = gate * sigma
    hidden = (active * upper).astype(jnp.bfloat16)
    d_up = (hidden_grad * active).astype(jnp.bfloat16)
    d_gate = (hidden_grad * upper * sigma * (1.0 + gate * (1.0 - sigma))).astype(jnp.bfloat16)
    factor = float(inputs.shape[0] * groups) ** (-0.5)
    owned = width // groups
    hunits = w_gate.shape[1]
    gate_local = jnp.einsum("td,tf->df", inputs, d_gate, preferred_element_type=single) * factor
    gate_parts = lax.all_to_all(
        gate_local.reshape(owned, groups, hunits).astype(jnp.bfloat16),
        "rep",
        split_axis=1,
        concat_axis=1,
        tiled=True,
    ).astype(jnp.float32)
    grad_gate = jnp.sum(gate_parts, axis=1, keepdims=True)
    up_local = jnp.einsum("td,tf->df", inputs, d_up, preferred_element_type=single) * factor
    up_parts = lax.all_to_all(
        up_local.reshape(owned, groups, hunits).astype(jnp.bfloat16),
        "rep",
        split_axis=1,
        concat_axis=1,
        tiled=True,
    ).astype(jnp.float32)
    grad_up = jnp.sum(up_parts, axis=1, keepdims=True)
    down_local = jnp.einsum("tf,td->fd", hidden, own_cot, preferred_element_type=single) * factor
    down_parts = lax.all_to_all(
        down_local.reshape(hunits, owned, groups).astype(jnp.bfloat16),
        "rep",
        split_axis=2,
        concat_axis=2,
        tiled=True,
    ).astype(jnp.float32)
    grad_down = jnp.sum(down_parts, axis=2, keepdims=True)
    input_term = jnp.einsum("tf,df->td", d_gate, w_gate, preferred_element_type=single)
    input_term = input_term + jnp.einsum("tf,df->td", d_up, w_up, preferred_element_type=single)
    grad_input = lax.psum(input_term.astype(jnp.bfloat16), "tp")
    gate_norms, up_norms = lax.psum(
        (jnp.sum(grad_gate * grad_gate, axis=2), jnp.sum(grad_up * grad_up, axis=2)), "tp"
    )
    down_norms = lax.psum(jnp.sum(grad_down * grad_down, axis=(1, 2)), ("rep", "fs"))
    return (grad_input, grad_gate, grad_up, grad_down, gate_norms, up_norms, down_norms)


def line_kernel(
    sizes, x_hbm, gate_hbm, up_hbm, cot_hbm, wg_hbm, wu_hbm, wd_hbm,
    gi_ref, gate_out, up_out, down_out, gu_norm_ref, down_norm_ref,
    x_ref, gate_ref, up_ref, cot_ref, wg_ref, wu_ref, wd_ref,
    left, left_far, right, right_far, pg_own, pg_peer, ab, sb, bb, gi_acc, gi_own, gi_peer,
    squares, gu_own, gu_peer, dn_own, dn_peer,
    load_sem, y_send, y_recv, a_send, a_recv, b_send, b_recv, c_send, c_recv,
    r_send, r_recv, f_send, f_recv, l_send, l_recv, m_send, m_recv,
    gi_send, gi_recv, gg_send, gg_recv, gn_send, gn_recv, dn_send, dn_recv,
):
    n_fs, n_tp, factor = sizes
    tokens, width = x_ref.shape
    hunits = gate_ref.shape[1]
    blocks = hunits // LANES
    items = 3 * blocks
    owned = width // 4
    share = tokens // n_tp
    rep, fs, tp = lax.axis_index("rep"), lax.axis_index("fs"), lax.axis_index("tp")
    side = rep // 2
    mid, end = 1 + side, 3 * side
    far_mid, far_end = 2 - side, 3 - 3 * side
    at_end = rep == end
    partner = mid + end - rep
    fs_peer = 1 - fs

    loads = [
        pltpu.make_async_copy(cot_hbm.at[:, pl.ds(pl.multiple_of(fs * width, LANES), width)], cot_ref, load_sem.at[0]),
        pltpu.make_async_copy(wd_hbm, wd_ref, load_sem.at[1]),
        pltpu.make_async_copy(gate_hbm, gate_ref, load_sem.at[2]),
        pltpu.make_async_copy(up_hbm, up_ref, load_sem.at[3]),
        pltpu.make_async_copy(x_hbm, x_ref, load_sem.at[4]),
        pltpu.make_async_copy(wg_hbm, wg_ref, load_sem.at[5]),
        pltpu.make_async_copy(wu_hbm, wu_ref, load_sem.at[6]),
    ]
    for load in loads:
        load.start()

    group = [(r, f) for r in range(4) for f in range(n_fs) if r or f]

    def in_group(step):
        return (lax.rem(rep + step[0], 4), lax.rem(fs + step[1], n_fs), tp)

    def in_tp(step):
        return (rep, fs, lax.rem(tp + step, n_tp))

    barrier = pltpu.get_barrier_semaphore()
    greeted = [in_group(s) for s in group] + [in_tp(s) for s in range(1, n_tp)]
    for other in greeted:
        pl.semaphore_signal(barrier, inc=1, device_id=other, device_id_type=MESH)
    pl.semaphore_wait(barrier, len(greeted))

    def remote(src, dst, send, recv, other):
        return pltpu.make_async_remote_copy(
            src_ref=src, dst_ref=dst, send_sem=send, recv_sem=recv, device_id=other, device_id_type=MESH
        )

    def y_copy(j):
        return remote(pg_own.at[j], pg_peer.at[j], y_send.at[j], y_recv.at[j], (rep, fs_peer, tp))

    def a_copy(t):
        return remote(ab.at[t], ab.at[t], a_send.at[t], a_recv.at[t], (partner, fs, tp))

    def b_copy(kind, t):
        src = ab.at[t, pl.ds(owned, 2 * owned)] if kind == 0 else sb.at[t - blocks]
        return remote(src, bb.at[t], b_send.at[t], b_recv.at[t], (far_mid, fs, tp))

    def c_copy(t):
        return remote(
            bb.at[t, pl.ds(owned, owned)], bb.at[t, pl.ds(0, owned)], c_send.at[t], c_recv.at[t], (partner, fs, tp)
        )

    half = tokens // n_fs
    own_half = pl.ds(pl.multiple_of(fs * half, 16), half)

    def r_copy(q):
        return remote(
            right.at[blocks + q, own_half], right_far.at[q, own_half], r_send.at[q], r_recv.at[q], (partner, fs, tp)
        )

    def f_copy(q):
        piece = right_far.at[q, own_half]
        return remote(piece, piece, f_send.at[q], f_recv.at[q], (rep, fs_peer, tp))

    piece_rows = 3 * owned // n_tp
    own_piece = pl.ds(pl.multiple_of(tp * piece_rows, 16), piece_rows)

    def l_copy():
        return remote(left.at[1, own_piece], left_far.at[own_piece], l_send.at[0], l_recv.at[0], (partner, fs, tp))

    def m_copy(step):
        piece = left_far.at[own_piece]
        return remote(piece, piece, m_send.at[step - 1], m_recv.at[step - 1], in_tp(step))

    def lanes(j):
        return pl.ds(pl.multiple_of(j * LANES, LANES), LANES)

    def rows_of(slot):
        return slice(slot * owned, (slot + 1) * owned)

    def term(kind, slot, t):
        return jnp.dot(left[kind, rows_of(slot), :], right[t], preferred_element_type=F32) * factor

    def long_term(slot, t):
        own = jnp.dot(left[1, rows_of(slot), :], right[t], preferred_element_type=F32)
        far = jnp.dot(left_far[rows_of(slot), :], right_far[t - blocks], preferred_element_type=F32)
        return (own + far) * factor

    def loop(first, last, body):
        def step(i, carry):
            body(i)
            return carry
        lax.fori_loop(first, last, step, 0)

    lead = min(3, blocks - 1)
    ahead = min(5, blocks)

    loads[0].wait()
    loads[1].wait()

    def partial_of(j):
        rows = pl.ds(pl.multiple_of(j * LANES, LANES), LANES)
        pg_own[j] = lax.dot_general(cot_ref[...], wd_ref[rows, :], NT, preferred_element_type=F32).astype(BF16)

        @pl.when(jnp.logical_or(at_end, j < ahead))
        def _():
            y_copy(j).start()

    loop(0, blocks, partial_of)

    def spread(kind, source):
        for slot, owner in enumerate((mid, far_mid, far_end, end)):
            place = lax.broadcasted_iota(jnp.int32, (owned, width), 0) * 4 + owner
            pick = (place == lax.broadcasted_iota(jnp.int32, (owned, width), 1)).astype(F32).astype(BF16)
            left[kind, rows_of(slot), :] = lax.dot_general(
                pick, source[...], NT, preferred_element_type=F32
            ).astype(BF16)

    spread(0, cot_ref)
    loads[2].wait()
    loads[3].wait()
    squares[...] = jnp.zeros_like(squares)
    dn_own[...] = jnp.zeros_like(dn_own)
    gu_own[...] = jnp.zeros_like(gu_own)

    def send_down(t):
        for slot in range(3):
            ab[t, rows_of(slot), :] = term(0, slot, t).astype(BF16)
        a_copy(t).start()

    def hidden_of(j):
        g = gate_ref[:, lanes(j)].astype(F32)
        u = up_ref[:, lanes(j)].astype(F32)
        right[j] = (g * (1.0 / (1.0 + jnp.exp(-g))) * u).astype(BF16)

    def hidden_first(j):
        hidden_of(j)

        @pl.when(at_end)
        def _():
            send_down(j)

    loop(0, 1, hidden_first)
    loads[4].wait()
    spread(1, x_ref)

    @pl.when(at_end)
    def _():
        l_copy().start()

    loop(1, lead, hidden_first)
    loop(lead, blocks, hidden_of)

    def grads_of(j):
        y_copy(j).wait_recv()
        g = gate_ref[:, lanes(j)].astype(F32)
        u = up_ref[:, lanes(j)].astype(F32)
        total = pg_own[j].astype(F32) + pg_peer[j].astype(F32)
        s = 1.0 / (1.0 + jnp.exp(-g))
        t = blocks + 2 * j
        right[t] = (total * u * s * (1.0 + g * (1.0 - s))).astype(BF16)
        right[t + 1] = (total * (g * s)).astype(BF16)

    def finish(kind, j, piece):
        if kind == 0:
            dn_own[0:1, lanes(j)] = jnp.sum(piece * piece, axis=0, keepdims=True)
            down_out[pl.ds(pl.multiple_of(j * LANES, LANES), LANES), 0, :] = piece.T
        else:
            squares[kind - 1] += piece * piece
            (gate_out if kind == 1 else up_out)[:, 0, lanes(j)] = piece

    def item(kind, j):
        return j if kind == 0 else blocks + 2 * j + kind - 1

    def down_on(t):
        a_copy(t).wait_recv()
        for slot in (1, 2):
            ab[t, rows_of(slot), :] = (ab[t, rows_of(slot), :].astype(F32) + term(0, slot, t)).astype(BF16)
        b_copy(0, t).start()

    def forward(j):
        for q in (2 * j, 2 * j + 1):
            r_copy(q).wait_recv()
            f_copy(q).start()

    def pair_on(j):
        for kind in (1, 2):
            t = item(kind, j)
            f_copy(t - blocks).wait_recv()
            for slot in (1, 2):
                sb[t - blocks, rows_of(slot - 1), :] = long_term(slot, t).astype(BF16)
            b_copy(kind, t).start()

    def settle(kind, j):
        t = item(kind, j)
        b_copy(kind, t).wait_recv()
        bb[t, owned:, :] = (bb[t, owned:, :].astype(F32) + term(min(kind, 1), 3, t)).astype(BF16)
        c_copy(t).start()
        if kind == 0:
            own = ab[t, :owned, :].astype(F32) + term(0, 0, t)
        else:
            own = long_term(0, t)
        finish(kind, j, own + bb[t, :owned, :].astype(F32))

    def last_hop(kind, j):
        t = item(kind, j)
        c_copy(t).wait_recv()
        finish(kind, j, bb[t, :owned, :].astype(F32) + term(min(kind, 1), 3, t))

    def through(action, j, with_down=True):
        action(1, j)
        action(2, j)
        if with_down:
            action(0, j + lead)

    downs = blocks - lead
    early = blocks - ahead

    @pl.when(at_end)
    def _():
        def pair_out(j):
            grads_of(j)
            r_copy(2 * j).start()
            r_copy(2 * j + 1).start()

        def both_out(j):
            pair_out(j)
            send_down(j + lead)

        loop(0, downs, both_out)
        loop(downs, blocks, pair_out)

    @pl.when(jnp.logical_not(at_end))
    def _():
        down_on(0)
        l_copy().wait_recv()
        for step in range(1, n_tp):
            m_copy(step).start()
        loop(1, lead, down_on)
        forward(0)
        for step in range(1, n_tp):
            m_copy(step).wait_recv()
        grads_of(0)
        forward(1)
        y_copy(ahead).start()
        pair_on(0)
        down_on(lead)
        loop(0, lead, functools.partial(settle, 0))

        def step(j):
            grads_of(j)
            forward(j + 1)
            y_copy(ahead + j).start()
            pair_on(j)
            down_on(j + lead)
            through(settle, j - 1)

        loop(1, early, step)
        loop(early, blocks, grads_of)

    loads[5].wait()
    loads[6].wait()
    gi_acc[...] = jnp.zeros_like(gi_acc)

    def gi_term(j):
        t = blocks + 2 * j
        gi_acc[...] += lax.dot_general(right[t], wg_ref[:, lanes(j)], NT, preferred_element_type=F32) + lax.dot_general(
            right[t + 1], wu_ref[:, lanes(j)], NT, preferred_element_type=F32
        )

    loop(0, blocks, gi_term)
    gi_own[...] = gi_acc[...].astype(BF16)

    def tokens_of(owner):
        return pl.ds(pl.multiple_of(owner * share, share), share)

    def gi_copy(step):
        other = lax.rem(tp + step, n_tp)
        return remote(
            gi_own.at[tokens_of(other)], gi_peer.at[step - 1], gi_send.at[step - 1], gi_recv.at[step - 1], in_tp(step)
        )

    def gg_copy(step):
        return remote(
            gi_ref.at[tokens_of(tp)], gi_ref.at[tokens_of(tp)], gg_send.at[step - 1], gg_recv.at[step - 1], in_tp(step)
        )

    for step in range(1, n_tp):
        gi_copy(step).start()

    @pl.when(at_end)
    def _():
        loop(0, lead, functools.partial(last_hop, 0))
        loop(0, downs, functools.partial(through, last_hop))

    @pl.when(jnp.logical_not(at_end))
    def _():
        def step(j):
            forward(j + 1)
            pair_on(j)
            down_on(j + lead)
            through(settle, j - 1)

        loop(early, downs, step)
        forward(downs + 1)
        pair_on(downs)
        through(settle, downs - 1)

    def dn_copy(k):
        return remote(dn_own, dn_peer.at[k], dn_send.at[k], dn_recv.at[k], in_group(group[k]))

    for k in range(len(group)):
        dn_copy(k).start()

    for step in range(1, n_tp):
        gi_copy(step).wait_recv()
    whole = gi_own[tokens_of(tp), :].astype(F32)
    for step in range(1, n_tp):
        whole += gi_peer[step - 1].astype(F32)
    gi_ref[tokens_of(tp), :] = whole.astype(BF16)
    for step in range(1, n_tp):
        gg_copy(step).start()

    @pl.when(at_end)
    def _():
        loop(downs, blocks, functools.partial(through, last_hop, with_down=False))

    @pl.when(jnp.logical_not(at_end))
    def _():
        def step(j):
            forward(j + 1)
            pair_on(j)
            through(settle, j - 1, with_down=False)

        loop(downs + 1, blocks - 1, step)
        pair_on(blocks - 1)
        through(settle, blocks - 2, with_down=False)
        through(settle, blocks - 1, with_down=False)

    for kind in range(2):
        gu_own[kind:kind + 1, :] = jnp.sum(squares[kind].T, axis=0, keepdims=True)

    def gn_copy(step):
        return remote(gu_own, gu_peer.at[step - 1], gn_send.at[step - 1], gn_recv.at[step - 1], in_tp(step))

    for step in range(1, n_tp):
        gn_copy(step).start()

    for k in range(len(group)):
        dn_copy(k).wait_recv()
    down = dn_own[...]
    for k in range(len(group)):
        down += dn_peer[k]
    down_norm_ref[...] = down

    for step in range(1, n_tp):
        gn_copy(step).wait_recv()
    gate_up = gu_own[...]
    for step in range(1, n_tp):
        gate_up += gu_peer[step - 1]
    gu_norm_ref[...] = gate_up

    for step in range(1, n_tp):
        gg_copy(step).wait_recv()
        gg_copy(step).wait_send()
        gi_copy(step).wait_send()
        gn_copy(step).wait_send()
    for k in range(len(group)):
        dn_copy(k).wait_send()
    loop(0, blocks, lambda j: y_copy(j).wait_send())

    @pl.when(at_end)
    def _():
        l_copy().wait_send()
        loop(0, blocks, lambda t: a_copy(t).wait_send())
        loop(0, 2 * blocks, lambda q: r_copy(q).wait_send())

    @pl.when(jnp.logical_not(at_end))
    def _():
        for step in range(1, n_tp):
            m_copy(step).wait_send()
        loop(0, blocks, lambda t: b_copy(0, t).wait_send())
        loop(blocks, items, lambda t: b_copy(1, t).wait_send())
        loop(0, items, lambda t: c_copy(t).wait_send())
        loop(0, 2 * blocks, lambda q: f_copy(q).wait_send())


def on_line(inputs, gate_pre, up_pre, cotangent, w_gate, w_up, w_down):
    n_fs, n_tp = lax.axis_size("fs"), lax.axis_size("tp")
    tokens, width = inputs.shape
    hunits = w_gate.shape[1]
    blocks = hunits // LANES
    items = 3 * blocks
    owned = width // 4
    share = tokens // n_tp
    n_group = 4 * n_fs - 1
    dma = pltpu.SemaphoreType.DMA
    vmem = pltpu.VMEM
    sizes = (n_fs, n_tp, float(tokens * 4) ** (-0.5))
    grad_input, grad_gate, grad_up, grad_down, gate_up, down = pl.pallas_call(
        functools.partial(line_kernel, sizes),
        out_shape=(
            jax.ShapeDtypeStruct((tokens, width), BF16),
            jax.ShapeDtypeStruct((owned, 1, hunits), F32),
            jax.ShapeDtypeStruct((owned, 1, hunits), F32),
            jax.ShapeDtypeStruct((hunits, 1, owned), F32),
            jax.ShapeDtypeStruct((8, owned), F32),
            jax.ShapeDtypeStruct((8, hunits), F32),
        ),
        in_specs=[pl.BlockSpec(memory_space=pl.ANY)] * 7,
        out_specs=(pl.BlockSpec(memory_space=vmem),) * 6,
        scratch_shapes=[
            vmem((tokens, width), BF16),
            vmem((tokens, hunits), BF16),
            vmem((tokens, hunits), BF16),
            vmem((tokens, width), BF16),
            vmem((width, hunits), BF16),
            vmem((width, hunits), BF16),
            vmem((hunits, width), BF16),
            vmem((2, width, tokens), BF16),
            vmem((3 * owned, tokens), BF16),
            vmem((items, tokens, LANES), BF16),
            vmem((2 * blocks, tokens, LANES), BF16),
            vmem((blocks, tokens, LANES), BF16),
            vmem((blocks, tokens, LANES), BF16),
            vmem((blocks, 3 * owned, LANES), BF16),
            vmem((2 * blocks, 2 * owned, LANES), BF16),
            vmem((items, 2 * owned, LANES), BF16),
            vmem((tokens, width), F32),
            vmem((tokens, width), BF16),
            vmem((n_tp - 1, share, width), BF16),
            vmem((2, owned, LANES), F32),
            vmem((8, owned), F32),
            vmem((n_tp - 1, 8, owned), F32),
            vmem((8, hunits), F32),
            vmem((n_group, 8, hunits), F32),
            dma((7,)),
            dma((blocks,)), dma((blocks,)),
            dma((blocks,)), dma((blocks,)),
            dma((items,)), dma((items,)),
            dma((items,)), dma((items,)),
            dma((2 * blocks,)), dma((2 * blocks,)),
            dma((2 * blocks,)), dma((2 * blocks,)),
            dma((1,)), dma((1,)),
            dma((n_tp - 1,)), dma((n_tp - 1,)),
            dma((n_tp - 1,)), dma((n_tp - 1,)),
            dma((n_tp - 1,)), dma((n_tp - 1,)),
            dma((n_tp - 1,)), dma((n_tp - 1,)),
            dma((n_group,)), dma((n_group,)),
        ],
        compiler_params=pltpu.CompilerParams(
            collective_id=0, has_side_effects=True, vmem_limit_bytes=67043328
        ),
    )(inputs, gate_pre, up_pre, cotangent, w_gate, w_up, w_down)
    return (
        grad_input,
        grad_gate,
        grad_up,
        grad_down.transpose(0, 2, 1),
        gate_up[0].reshape(owned, 1),
        gate_up[1].reshape(owned, 1),
        down[0],
    )


def fits_line(mesh, inputs, w_gate):
    n_rep, n_fs, n_tp = (mesh.shape[axis] for axis in ("rep", "fs", "tp"))
    tokens, width = inputs.shape[0] // n_rep, inputs.shape[1] // n_fs
    return (
        n_rep == 4 and n_fs == 2 and n_tp > 1 and w_gate.shape[1] // n_tp >= 10 * LANES
        and (3 * width // 4) % (16 * n_tp) == 0
        and tokens % (16 * n_tp) == 0 and tokens % LANES == 0
        and width % (4 * LANES) == 0 and (w_gate.shape[1] // n_tp) % LANES == 0
    )


def solution(mesh):
    placed = (
        P("rep", "fs"),
        P("rep", "tp"),
        P("rep", "tp"),
        P("rep", None),
        P("fs", "tp"),
        P("fs", "tp"),
        P("tp", "fs"),
    )
    out_placed = (
        P("rep", "fs"),
        P("fs", "rep", "tp"),
        P("fs", "rep", "tp"),
        P("tp", "fs", "rep"),
        P("fs", "rep"),
        P("fs", "rep"),
        P("tp"),
    )

    def whole(inputs, gate_pre, up_pre, cotangent, w_gate, w_up, w_down):
        body = on_line if fits_line(mesh, inputs, w_gate) else on_device
        mapped = jax.shard_map(body, mesh=mesh, in_specs=placed, out_specs=out_placed, check_vma=False)
        return mapped(inputs, gate_pre, up_pre, cotangent, w_gate, w_up, w_down)

    return whole
```

```python
import functools

import jax
import jax.numpy as jnp
from jax import lax
from jax.experimental import pallas as pl
from jax.experimental.pallas import tpu as pltpu
from jax.sharding import PartitionSpec as P

LANES = 128
F32 = jnp.float32
BF16 = jnp.bfloat16
MESH = pl.DeviceIdType.MESH
NT = (((1,), (1,)), ((), ()))


def on_device(inputs, gate_pre, up_pre, cotangent, w_gate, w_up, w_down):
    single = jnp.float32
    groups = lax.axis_size("rep")
    width = w_down.shape[1]
    own_cot = lax.dynamic_slice_in_dim(cotangent, lax.axis_index("fs") * width, width, 1)
    partial_grad = jnp.einsum("td,fd->tf", own_cot, w_down, preferred_element_type=single)
    hidden_grad = lax.psum(partial_grad.astype(jnp.bfloat16), "fs").astype(jnp.float32)
    gate = gate_pre.astype(single)
    upper = up_pre.astype(single)
    sigma = jax.nn.sigmoid(gate)
    active = gate * sigma
    hidden = (active * upper).astype(jnp.bfloat16)
    d_up = (hidden_grad * active).astype(jnp.bfloat16)
    d_gate = (hidden_grad * upper * sigma * (1.0 + gate * (1.0 - sigma))).astype(jnp.bfloat16)
    factor = float(inputs.shape[0] * groups) ** (-0.5)
    owned = width // groups
    hunits = w_gate.shape[1]
    gate_local = jnp.einsum("td,tf->df", inputs, d_gate, preferred_element_type=single) * factor
    gate_parts = lax.all_to_all(
        gate_local.reshape(owned, groups, hunits).astype(jnp.bfloat16),
        "rep",
        split_axis=1,
        concat_axis=1,
        tiled=True,
    ).astype(jnp.float32)
    grad_gate = jnp.sum(gate_parts, axis=1, keepdims=True)
    up_local = jnp.einsum("td,tf->df", inputs, d_up, preferred_element_type=single) * factor
    up_parts = lax.all_to_all(
        up_local.reshape(owned, groups, hunits).astype(jnp.bfloat16),
        "rep",
        split_axis=1,
        concat_axis=1,
        tiled=True,
    ).astype(jnp.float32)
    grad_up = jnp.sum(up_parts, axis=1, keepdims=True)
    down_local = jnp.einsum("tf,td->fd", hidden, own_cot, preferred_element_type=single) * factor
    down_parts = lax.all_to_all(
        down_local.reshape(hunits, owned, groups).astype(jnp.bfloat16),
        "rep",
        split_axis=2,
        concat_axis=2,
        tiled=True,
    ).astype(jnp.float32)
    grad_down = jnp.sum(down_parts, axis=2, keepdims=True)
    input_term = jnp.einsum("tf,df->td", d_gate, w_gate, preferred_element_type=single)
    input_term = input_term + jnp.einsum("tf,df->td", d_up, w_up, preferred_element_type=single)
    grad_input = lax.psum(input_term.astype(jnp.bfloat16), "tp")
    gate_norms, up_norms = lax.psum(
        (jnp.sum(grad_gate * grad_gate, axis=2), jnp.sum(grad_up * grad_up, axis=2)), "tp"
    )
    down_norms = lax.psum(jnp.sum(grad_down * grad_down, axis=(1, 2)), ("rep", "fs"))
    return (grad_input, grad_gate, grad_up, grad_down, gate_norms, up_norms, down_norms)


def line_kernel(
    sizes, x_hbm, gate_hbm, up_hbm, cot_hbm, wg_hbm, wu_hbm, wd_hbm,
    gi_ref, gate_out, up_out, down_out, gu_norm_ref, down_norm_ref,
    x_ref, gate_ref, up_ref, cot_ref, wg_ref, wu_ref, wd_ref,
    left, left_far, right, right_far, pg_own, pg_peer, ab, sb, bb, gi_acc, gi_own, gi_peer,
    squares, gu_own, gu_peer, dn_own, dn_peer,
    load_sem, y_send, y_recv, a_send, a_recv, b_send, b_recv, c_send, c_recv,
    r_send, r_recv, f_send, f_recv, l_send, l_recv, m_send, m_recv,
    gi_send, gi_recv, gg_send, gg_recv, gn_send, gn_recv, dn_send, dn_recv,
):
    n_fs, n_tp, factor = sizes
    tokens, width = x_ref.shape
    hunits = gate_ref.shape[1]
    blocks = hunits // LANES
    items = 3 * blocks
    owned = width // 4
    share = tokens // n_tp
    rep, fs, tp = lax.axis_index("rep"), lax.axis_index("fs"), lax.axis_index("tp")
    side = rep // 2
    mid, end = 1 + side, 3 * side
    far_mid, far_end = 2 - side, 3 - 3 * side
    at_end = rep == end
    partner = mid + end - rep
    fs_peer = 1 - fs

    loads = [
        pltpu.make_async_copy(cot_hbm.at[:, pl.ds(pl.multiple_of(fs * width, LANES), width)], cot_ref, load_sem.at[0]),
        pltpu.make_async_copy(wd_hbm, wd_ref, load_sem.at[1]),
        pltpu.make_async_copy(gate_hbm, gate_ref, load_sem.at[2]),
        pltpu.make_async_copy(up_hbm, up_ref, load_sem.at[3]),
        pltpu.make_async_copy(x_hbm, x_ref, load_sem.at[4]),
        pltpu.make_async_copy(wg_hbm, wg_ref, load_sem.at[5]),
        pltpu.make_async_copy(wu_hbm, wu_ref, load_sem.at[6]),
    ]
    for k in (0, 2, 3, 4, 1, 5, 6):
        loads[k].start()

    group = [(r, f) for r in range(4) for f in range(n_fs) if r or f]

    def in_group(step):
        return (lax.rem(rep + step[0], 4), lax.rem(fs + step[1], n_fs), tp)

    def in_tp(step):
        return (rep, fs, lax.rem(tp + step, n_tp))

    barrier = pltpu.get_barrier_semaphore()
    greeted = [in_group(s) for s in group] + [in_tp(s) for s in range(1, n_tp)]
    for other in greeted:
        pl.semaphore_signal(barrier, inc=1, device_id=other, device_id_type=MESH)
    pl.semaphore_wait(barrier, len(greeted))

    def remote(src, dst, send, recv, other):
        return pltpu.make_async_remote_copy(
            src_ref=src, dst_ref=dst, send_sem=send, recv_sem=recv, device_id=other, device_id_type=MESH
        )

    def y_copy(j):
        return remote(pg_own.at[j], pg_peer.at[j], y_send.at[j], y_recv.at[j], (rep, fs_peer, tp))

    def a_copy(t):
        return remote(ab.at[t], ab.at[t], a_send.at[t], a_recv.at[t], (partner, fs, tp))

    def b_copy(kind, t):
        src = ab.at[t, pl.ds(owned, 2 * owned)] if kind == 0 else sb.at[t - blocks]
        return remote(src, bb.at[t], b_send.at[t], b_recv.at[t], (far_mid, fs, tp))

    def c_copy(t):
        return remote(
            bb.at[t, pl.ds(owned, owned)], bb.at[t, pl.ds(0, owned)], c_send.at[t], c_recv.at[t], (partner, fs, tp)
        )

    half = tokens // n_fs
    own_half = pl.ds(pl.multiple_of(fs * half, 16), half)

    def r_copy(q):
        return remote(
            right.at[blocks + q, own_half], right_far.at[q, own_half], r_send.at[q], r_recv.at[q], (partner, fs, tp)
        )

    def f_copy(q):
        piece = right_far.at[q, own_half]
        return remote(piece, piece, f_send.at[q], f_recv.at[q], (rep, fs_peer, tp))

    piece_rows = 3 * owned // n_tp
    own_piece = pl.ds(pl.multiple_of(tp * piece_rows, 16), piece_rows)

    def l_copy():
        return remote(left.at[1, own_piece], left_far.at[own_piece], l_send.at[0], l_recv.at[0], (partner, fs, tp))

    def m_copy(step):
        piece = left_far.at[own_piece]
        return remote(piece, piece, m_send.at[step - 1], m_recv.at[step - 1], in_tp(step))

    def lanes(j):
        return pl.ds(pl.multiple_of(j * LANES, LANES), LANES)

    def rows_of(slot):
        return slice(slot * owned, (slot + 1) * owned)

    def term(kind, slot, t):
        return jnp.dot(left[kind, rows_of(slot), :], right[t], preferred_element_type=F32) * factor

    def long_term(slot, t):
        own = jnp.dot(left[1, rows_of(slot), :], right[t], preferred_element_type=F32)
        far = jnp.dot(left_far[rows_of(slot), :], right_far[t - blocks], preferred_element_type=F32)
        return (own + far) * factor

    def loop(first, last, body):
        def step(i, carry):
            body(i)
            return carry
        lax.fori_loop(first, last, step, 0)

    lead = min(2, blocks - 1)
    ahead = min(5, blocks)

    def spread(kind, source):
        for slot, owner in enumerate((mid, far_mid, far_end, end)):
            place = lax.broadcasted_iota(jnp.int32, (owned, width), 0) * 4 + owner
            pick = (place == lax.broadcasted_iota(jnp.int32, (owned, width), 1)).astype(F32).astype(BF16)
            left[kind, rows_of(slot), :] = lax.dot_general(
                pick, source[...], NT, preferred_element_type=F32
            ).astype(BF16)

    loads[0].wait()
    spread(0, cot_ref)
    loads[2].wait()
    loads[3].wait()
    squares[...] = jnp.zeros_like(squares)
    dn_own[...] = jnp.zeros_like(dn_own)
    gu_own[...] = jnp.zeros_like(gu_own)

    def send_down(t):
        for slot in range(3):
            ab[t, rows_of(slot), :] = term(0, slot, t).astype(BF16)
        a_copy(t).start()

    def hidden_of(j):
        g = gate_ref[:, lanes(j)].astype(F32)
        u = up_ref[:, lanes(j)].astype(F32)
        right[j] = (g * (1.0 / (1.0 + jnp.exp(-g))) * u).astype(BF16)

    def hidden_first(j):
        hidden_of(j)

        @pl.when(at_end)
        def _():
            send_down(j)

    loop(0, 1, hidden_first)
    loads[4].wait()
    spread(1, x_ref)

    @pl.when(at_end)
    def _():
        l_copy().start()

    loop(1, lead, hidden_first)

    loads[1].wait()

    def partial_of(j):
        rows = pl.ds(pl.multiple_of(j * LANES, LANES), LANES)
        pg_own[j] = lax.dot_general(cot_ref[...], wd_ref[rows, :], NT, preferred_element_type=F32).astype(BF16)

        @pl.when(jnp.logical_or(at_end, j < ahead))
        def _():
            y_copy(j).start()

    loop(0, blocks, partial_of)

    loop(lead, blocks, hidden_of)

    def grads_of(j):
        y_copy(j).wait_recv()
        g = gate_ref[:, lanes(j)].astype(F32)
        u = up_ref[:, lanes(j)].astype(F32)
        total = pg_own[j].astype(F32) + pg_peer[j].astype(F32)
        s = 1.0 / (1.0 + jnp.exp(-g))
        t = blocks + 2 * j
        right[t] = (total * u * s * (1.0 + g * (1.0 - s))).astype(BF16)
        right[t + 1] = (total * (g * s)).astype(BF16)

    def finish(kind, j, piece):
        if kind == 0:
            dn_own[0:1, lanes(j)] = jnp.sum(piece * piece, axis=0, keepdims=True)
            down_out[pl.ds(pl.multiple_of(j * LANES, LANES), LANES), 0, :] = piece.T
        else:
            squares[kind - 1] += piece * piece
            (gate_out if kind == 1 else up_out)[:, 0, lanes(j)] = piece

    def item(kind, j):
        return j if kind == 0 else blocks + 2 * j + kind - 1

    def down_on(t):
        a_copy(t).wait_recv()
        for slot in (1, 2):
            ab[t, rows_of(slot), :] = (ab[t, rows_of(slot), :].astype(F32) + term(0, slot, t)).astype(BF16)
        b_copy(0, t).start()

    def forward(j):
        for q in (2 * j, 2 * j + 1):
            r_copy(q).wait_recv()
            f_copy(q).start()

    def pair_on(j):
        for kind in (1, 2):
            t = item(kind, j)
            f_copy(t - blocks).wait_recv()
            for slot in (1, 2):
                sb[t - blocks, rows_of(slot - 1), :] = long_term(slot, t).astype(BF16)
            b_copy(kind, t).start()

    def settle(kind, j):
        t = item(kind, j)
        b_copy(kind, t).wait_recv()
        bb[t, owned:, :] = (bb[t, owned:, :].astype(F32) + term(min(kind, 1), 3, t)).astype(BF16)
        c_copy(t).start()
        if kind == 0:
            own = ab[t, :owned, :].astype(F32) + term(0, 0, t)
        else:
            own = long_term(0, t)
        finish(kind, j, own + bb[t, :owned, :].astype(F32))

    def last_hop(kind, j):
        t = item(kind, j)
        c_copy(t).wait_recv()
        finish(kind, j, bb[t, :owned, :].astype(F32) + term(min(kind, 1), 3, t))

    def through(action, j, with_down=True):
        action(1, j)
        action(2, j)
        if with_down:
            action(0, j + lead)

    def gi_term(j):
        t = blocks + 2 * j
        gi_acc[...] += lax.dot_general(right[t], wg_ref[:, lanes(j)], NT, preferred_element_type=F32) + lax.dot_general(
            right[t + 1], wu_ref[:, lanes(j)], NT, preferred_element_type=F32
        )

    def grads_and_term(j):
        grads_of(j)
        gi_term(j)

    gi_acc[...] = jnp.zeros_like(gi_acc)
    downs = blocks - lead
    early = blocks - ahead

    @pl.when(at_end)
    def _():
        def pair_out(j):
            grads_of(j)
            r_copy(2 * j).start()
            r_copy(2 * j + 1).start()

        def both_out(j):
            pair_out(j)
            send_down(j + lead)

        loop(0, downs, both_out)
        loop(downs, blocks, pair_out)
        loads[5].wait()
        loads[6].wait()
        loop(0, blocks, gi_term)

    @pl.when(jnp.logical_not(at_end))
    def _():
        loads[5].wait()
        loads[6].wait()
        down_on(0)
        l_copy().wait_recv()
        for step in range(1, n_tp):
            m_copy(step).start()
        loop(1, lead, down_on)
        forward(0)
        for step in range(1, n_tp):
            m_copy(step).wait_recv()
        grads_and_term(0)
        forward(1)
        y_copy(ahead).start()
        pair_on(0)
        down_on(lead)
        loop(0, lead, functools.partial(settle, 0))

        def step(j):
            grads_of(j)
            forward(j + 1)
            y_copy(ahead + j).start()
            pair_on(j)
            down_on(j + lead)
            gi_term(j)
            through(settle, j - 1)

            @pl.when(j > 1)
            def _():
                grads_and_term(ahead - 1 + j)

        loop(1, early, step)
        loop(ahead - 1 + early, blocks, grads_and_term)

    gi_own[...] = gi_acc[...].astype(BF16)

    def tokens_of(owner):
        return pl.ds(pl.multiple_of(owner * share, share), share)

    def gi_copy(step):
        other = lax.rem(tp + step, n_tp)
        return remote(
            gi_own.at[tokens_of(other)], gi_peer.at[step - 1], gi_send.at[step - 1], gi_recv.at[step - 1], in_tp(step)
        )

    def gg_copy(step):
        return remote(
            gi_ref.at[tokens_of(tp)], gi_ref.at[tokens_of(tp)], gg_send.at[step - 1], gg_recv.at[step - 1], in_tp(step)
        )

    for step in range(1, n_tp):
        gi_copy(step).start()

    @pl.when(at_end)
    def _():
        loop(0, lead, functools.partial(last_hop, 0))
        loop(0, downs, functools.partial(through, last_hop))

    @pl.when(jnp.logical_not(at_end))
    def _():
        def step(j):
            forward(j + 1)
            pair_on(j)
            down_on(j + lead)
            through(settle, j - 1)

        loop(early, downs, step)
        forward(downs + 1)
        pair_on(downs)
        through(settle, downs - 1)

    def dn_copy(k):
        return remote(dn_own, dn_peer.at[k], dn_send.at[k], dn_recv.at[k], in_group(group[k]))

    for k in range(len(group)):
        dn_copy(k).start()

    for step in range(1, n_tp):
        gi_copy(step).wait_recv()
    whole = gi_own[tokens_of(tp), :].astype(F32)
    for step in range(1, n_tp):
        whole += gi_peer[step - 1].astype(F32)
    gi_ref[tokens_of(tp), :] = whole.astype(BF16)
    for step in range(1, n_tp):
        gg_copy(step).start()

    @pl.when(at_end)
    def _():
        loop(downs, blocks, functools.partial(through, last_hop, with_down=False))

    @pl.when(jnp.logical_not(at_end))
    def _():
        def step(j):
            forward(j + 1)
            pair_on(j)
            through(settle, j - 1, with_down=False)

        loop(downs + 1, blocks - 1, step)
        pair_on(blocks - 1)
        through(settle, blocks - 2, with_down=False)
        through(settle, blocks - 1, with_down=False)

    for kind in range(2):
        gu_own[kind:kind + 1, :] = jnp.sum(squares[kind].T, axis=0, keepdims=True)

    def gn_copy(step):
        return remote(gu_own, gu_peer.at[step - 1], gn_send.at[step - 1], gn_recv.at[step - 1], in_tp(step))

    for step in range(1, n_tp):
        gn_copy(step).start()

    for k in range(len(group)):
        dn_copy(k).wait_recv()
    down = dn_own[...]
    for k in range(len(group)):
        down += dn_peer[k]
    down_norm_ref[...] = down

    for step in range(1, n_tp):
        gn_copy(step).wait_recv()
    gate_up = gu_own[...]
    for step in range(1, n_tp):
        gate_up += gu_peer[step - 1]
    gu_norm_ref[...] = gate_up

    for step in range(1, n_tp):
        gg_copy(step).wait_recv()
        gg_copy(step).wait_send()
        gi_copy(step).wait_send()
        gn_copy(step).wait_send()
    for k in range(len(group)):
        dn_copy(k).wait_send()
    loop(0, blocks, lambda j: y_copy(j).wait_send())

    @pl.when(at_end)
    def _():
        l_copy().wait_send()
        loop(0, blocks, lambda t: a_copy(t).wait_send())
        loop(0, 2 * blocks, lambda q: r_copy(q).wait_send())

    @pl.when(jnp.logical_not(at_end))
    def _():
        for step in range(1, n_tp):
            m_copy(step).wait_send()
        loop(0, blocks, lambda t: b_copy(0, t).wait_send())
        loop(blocks, items, lambda t: b_copy(1, t).wait_send())
        loop(0, items, lambda t: c_copy(t).wait_send())
        loop(0, 2 * blocks, lambda q: f_copy(q).wait_send())


def on_line(inputs, gate_pre, up_pre, cotangent, w_gate, w_up, w_down):
    n_fs, n_tp = lax.axis_size("fs"), lax.axis_size("tp")
    tokens, width = inputs.shape
    hunits = w_gate.shape[1]
    blocks = hunits // LANES
    items = 3 * blocks
    owned = width // 4
    share = tokens // n_tp
    n_group = 4 * n_fs - 1
    dma = pltpu.SemaphoreType.DMA
    vmem = pltpu.VMEM
    sizes = (n_fs, n_tp, float(tokens * 4) ** (-0.5))
    grad_input, grad_gate, grad_up, grad_down, gate_up, down = pl.pallas_call(
        functools.partial(line_kernel, sizes),
        out_shape=(
            jax.ShapeDtypeStruct((tokens, width), BF16),
            jax.ShapeDtypeStruct((owned, 1, hunits), F32),
            jax.ShapeDtypeStruct((owned, 1, hunits), F32),
            jax.ShapeDtypeStruct((hunits, 1, owned), F32),
            jax.ShapeDtypeStruct((8, owned), F32),
            jax.ShapeDtypeStruct((8, hunits), F32),
        ),
        in_specs=[pl.BlockSpec(memory_space=pl.ANY)] * 7,
        out_specs=(pl.BlockSpec(memory_space=vmem),) * 6,
        scratch_shapes=[
            vmem((tokens, width), BF16),
            vmem((tokens, hunits), BF16),
            vmem((tokens, hunits), BF16),
            vmem((tokens, width), BF16),
            vmem((width, hunits), BF16),
            vmem((width, hunits), BF16),
            vmem((hunits, width), BF16),
            vmem((2, width, tokens), BF16),
            vmem((3 * owned, tokens), BF16),
            vmem((items, tokens, LANES), BF16),
            vmem((2 * blocks, tokens, LANES), BF16),
            vmem((blocks, tokens, LANES), BF16),
            vmem((blocks, tokens, LANES), BF16),
            vmem((blocks, 3 * owned, LANES), BF16),
            vmem((2 * blocks, 2 * owned, LANES), BF16),
            vmem((items, 2 * owned, LANES), BF16),
            vmem((tokens, width), F32),
            vmem((tokens, width), BF16),
            vmem((n_tp - 1, share, width), BF16),
            vmem((2, owned, LANES), F32),
            vmem((8, owned), F32),
            vmem((n_tp - 1, 8, owned), F32),
            vmem((8, hunits), F32),
            vmem((n_group, 8, hunits), F32),
            dma((7,)),
            dma((blocks,)), dma((blocks,)),
            dma((blocks,)), dma((blocks,)),
            dma((items,)), dma((items,)),
            dma((items,)), dma((items,)),
            dma((2 * blocks,)), dma((2 * blocks,)),
            dma((2 * blocks,)), dma((2 * blocks,)),
            dma((1,)), dma((1,)),
            dma((n_tp - 1,)), dma((n_tp - 1,)),
            dma((n_tp - 1,)), dma((n_tp - 1,)),
            dma((n_tp - 1,)), dma((n_tp - 1,)),
            dma((n_tp - 1,)), dma((n_tp - 1,)),
            dma((n_group,)), dma((n_group,)),
        ],
        compiler_params=pltpu.CompilerParams(
            collective_id=0, has_side_effects=True, vmem_limit_bytes=67043328
        ),
    )(inputs, gate_pre, up_pre, cotangent, w_gate, w_up, w_down)
    return (
        grad_input,
        grad_gate,
        grad_up,
        grad_down.transpose(0, 2, 1),
        gate_up[0].reshape(owned, 1),
        gate_up[1].reshape(owned, 1),
        down[0],
    )


def fits_line(mesh, inputs, w_gate):
    n_rep, n_fs, n_tp = (mesh.shape[axis] for axis in ("rep", "fs", "tp"))
    tokens, width = inputs.shape[0] // n_rep, inputs.shape[1] // n_fs
    return (
        n_rep == 4 and n_fs == 2 and n_tp > 1 and w_gate.shape[1] // n_tp >= 10 * LANES
        and (3 * width // 4) % (16 * n_tp) == 0
        and tokens % (16 * n_tp) == 0 and tokens % LANES == 0
        and width % (4 * LANES) == 0 and (w_gate.shape[1] // n_tp) % LANES == 0
    )


def solution(mesh):
    placed = (
        P("rep", "fs"),
        P("rep", "tp"),
        P("rep", "tp"),
        P("rep", None),
        P("fs", "tp"),
        P("fs", "tp"),
        P("tp", "fs"),
    )
    out_placed = (
        P("rep", "fs"),
        P("fs", "rep", "tp"),
        P("fs", "rep", "tp"),
        P("tp", "fs", "rep"),
        P("fs", "rep"),
        P("fs", "rep"),
        P("tp"),
    )

    def whole(inputs, gate_pre, up_pre, cotangent, w_gate, w_up, w_down):
        body = on_line if fits_line(mesh, inputs, w_gate) else on_device
        mapped = jax.shard_map(body, mesh=mesh, in_specs=placed, out_specs=out_placed, check_vma=False)
        return mapped(inputs, gate_pre, up_pre, cotangent, w_gate, w_up, w_down)

    return whole
```
